32 devices in a mesh: sp: 4 (over z), fs: 4 (over y, x), tp: 2 (over core).
Axes of the slice: x: 2, y: 2, z: 4, core: 2. Of those that a mesh axis runs over, the one named last changes fastest.
Arguments:
- tokens: bfloat16 [4, 1024, 2048], P('fs', 'sp', 'tp'), may hold values from -6 to 6
- norm_gain: float32 [2048], replicated, may hold values from 0.1 to 1.9
- query_weight: bfloat16 [2048, 1024], P('fs', 'tp'), may hold values from -1 to 1
- key_weight: bfloat16 [2048, 1024], P('fs', 'tp'), may hold values from -4 to 4
- value_weight: bfloat16 [2048, 1024], P('fs', 'tp'), may hold values from -0.125 to 0.125
- state_query: bfloat16 [2048, 1024], P('fs', 'tp'), may hold values from -0.125 to 0.125
- state_key: bfloat16 [2048, 1024], P('fs', 'tp'), may hold values from -0.125 to 0.125
- state_value: bfloat16 [2048, 1024], P('fs', 'tp'), may hold values from -0.125 to 0.125
- map_lambda: float32 [8], P('tp'), may hold values from 0.3 to 0.8
- diff_gain: float32 [1024], P('tp'), may hold values from 0.1 to 1.9
- decay_rate: float32 [8], P('tp'), may hold values from 0 to 0.04
- state_gain: float32 [1024], P('tp'), may hold values from 0.1 to 1.9
- out_weight: bfloat16 [2048, 2048], replicated, may hold values from -0.125 to 0.125
Outputs:
- mixed: bfloat16 [4, 1024, 2048], P('fs', ('sp', 'tp'))
The draws below stay inside these ranges and needn't reach their ends.
All inputs are finite; a program needn't handle non-finite values.
Results may differ from the reference program's by a relative error of at most 0.015.
Values may be sent and summed in bfloat16 or wider, within the bound.
A program may use at most 128 MiB of HBM per device.

```python
import math
import jax
import jax.numpy as jnp
from jax import lax

D = 2048
HD = 8
DK = 64
DV = 128
HR = 8
DR = 128
TOK_DEV = 256
LENGTH = 1024
SEQS = 4


def query_base(key):
    return jax.random.normal(jax.random.fold_in(key, 101), (D, HD * 2 * DK), jnp.float32) * (2.0 / D) ** 0.5


def draw_query_weight(key, part):
    return jnp.clip(query_base(key), -1.0, 1.0).astype(jnp.bfloat16)


def draw_key_weight(key, part):
    fresh = jax.random.normal(jax.random.fold_in(key, 202), (D, HD * 2 * DK), jnp.float32) * (2.0 / D) ** 0.5
    result = fresh
    return jnp.clip(result, -4.0, 4.0).astype(jnp.bfloat16)


def draw_decay_rate(key, part):
    pick = jax.random.uniform(jax.random.fold_in(key, 404), (HR,), jnp.float32)
    share = 0.5
    slow_rate = jnp.exp(jax.random.uniform(jax.random.fold_in(key, 505), (HR,), jnp.float32, math.log(0.1), math.log(2.0))) / LENGTH
    fast_rate = jnp.exp(jax.random.uniform(jax.random.fold_in(key, 606), (HR,), jnp.float32, math.log(0.01), math.log(0.033)))
    return jnp.where(pick < share, slow_rate, fast_rate)


def shard_levels(key, shape, pieces, smallest, high):
    level, own = 1.0, jax.random.fold_in(key, 6)
    for dim, blocks in pieces:
        steps = jnp.exp(jax.random.uniform(jax.random.fold_in(own, dim), (blocks,), jnp.float32, smallest / len(pieces), high / len(pieces)))
        level = level * jnp.repeat(steps, shape[dim] // blocks).reshape([-1 if axis == dim else 1 for axis in range(len(shape))])
    return level


def scatter_about(rng, dims, width, most, shards=(), held_as=jnp.bfloat16):
    drawn = width * jax.random.normal(rng, dims, jnp.float32)
    if shards:
        drawn = drawn * shard_levels(rng, dims, shards, -0.22, 0.18)
    return jnp.clip(drawn, -most, most).astype(held_as)


def setup_inputs(seed: int = 0) -> dict:
    key_list = jax.random.split(jax.random.key(seed), 14)
    return {
        "tokens": scatter_about(key_list[0], (SEQS, LENGTH, D), 1.0, 6.0, ((0, 4), (1, 4), (2, 2))),
        "norm_gain": jnp.clip(1.0 + 0.18 * jax.random.normal(key_list[1], (D,), jnp.float32), 0.1, 1.9),
        "query_weight": draw_query_weight(jax.random.fold_in(key_list[13], 71), 0),
        "key_weight": draw_key_weight(jax.random.fold_in(key_list[13], 71), 0),
        "value_weight": scatter_about(key_list[4], (D, HD * DV), D ** -0.5, 0.125, ((0, 4), (1, 2))),
        "state_query": scatter_about(key_list[5], (D, HR * DR), D ** -0.5, 0.125, ((0, 4), (1, 2))),
        "state_key": scatter_about(key_list[6], (D, HR * DR), D ** -0.5, 0.125, ((0, 4), (1, 2))),
        "state_value": scatter_about(key_list[7], (D, HR * DR), D ** -0.5, 0.125, ((0, 4), (1, 2))),
        "map_lambda": jnp.clip(0.3 + 0.5 * jax.random.uniform(key_list[8], (HD,), jnp.float32) ** shard_levels(key_list[8], (HD,), ((0, 2),), -0.2, 0.2), 0.3, 0.8),
        "diff_gain": jnp.clip(1.0 + 0.18 * jax.random.normal(key_list[9], (HD * DV,), jnp.float32), 0.1, 1.9),
        "decay_rate": draw_decay_rate(jax.random.fold_in(key_list[13], 71), 0),
        "state_gain": jnp.clip(1.0 + 0.18 * jax.random.normal(key_list[11], (HR * DR,), jnp.float32), 0.1, 1.9),
        "out_weight": scatter_about(key_list[12], (HD * DV + HR * DR, D), (HD * DV + HR * DR) ** -0.5, 0.125),
    }


epsilon = 1e-05
branch_scale = 0.8
masked_score = -1e+30

def normalize(values, gain):
    meansq = lax.optimization_barrier(jnp.mean(values * values, axis=-1, keepdims=True))
    return values * lax.rsqrt(meansq + epsilon) * gain

def rounded(values):
    return lax.optimization_barrier(values.astype(jnp.bfloat16)).astype(jnp.float32)

def differential(att_query, att_keys, att_values, map_lambda, diff_gain):
    length = att_query.shape[0]
    blocks = length // TOK_DEV
    query_float = att_query.reshape(blocks, TOK_DEV, HD, 2, DK).astype(jnp.float32)
    key_float = att_keys.reshape(length, HD, 2, DK).astype(jnp.float32)
    value_float = att_values.reshape(length, HD, DV).astype(jnp.float32)
    key_place = jnp.arange(length)

    def one_block(inputs):
        block_index, query_block = inputs
        query_place = block_index * TOK_DEV + jnp.arange(TOK_DEV)
        scores = jnp.einsum('qhmd,khmd->mhqk', query_block, key_float) * DK ** (-0.5)
        causal = key_place[None, :] <= query_place[:, None]
        row_peak = lax.optimization_barrier(jnp.max(jnp.where(causal, scores, masked_score), axis=-1, keepdims=True))
        weights = jnp.where(causal, jnp.exp(scores - row_peak), 0.0)
        totals = lax.optimization_barrier(jnp.sum(weights, axis=-1, keepdims=True))
        averaged = jnp.einsum('mhqk,khv->mhqv', rounded(weights), value_float) / totals
        differ = averaged[0] - map_lambda[:, None, None] * averaged[1]
        normed = normalize(differ, diff_gain.reshape(HD, 1, DV)) * branch_scale
        return normed.transpose(1, 0, 2).reshape(TOK_DEV, HD * DV).astype(jnp.bfloat16)
    outputs = lax.map(one_block, (jnp.arange(blocks), query_float))
    return outputs.reshape(length, HD * DV)

def retention(ret_query, ret_keys, ret_values, decay_rate, state_gain):
    length = ret_query.shape[0]
    blocks = length // TOK_DEV

    def to_blocks(array):
        return array.reshape(blocks, TOK_DEV, HR, DR)
    position = jnp.arange(TOK_DEV).astype(jnp.float32)
    distance = position[:, None] - position[None, :]
    decay_col = decay_rate[:, None, None]
    within = jnp.where(distance >= 0, jnp.exp(-decay_col * jnp.maximum(distance, 0.0)), 0.0)
    query_decay = jnp.exp(-decay_col * (position + 1.0)[None, :, None])
    key_decay = jnp.exp(-decay_rate[None, :, None] * (TOK_DEV - 1.0 - position)[:, None, None])
    block_decay = jnp.exp(-decay_rate * TOK_DEV)[:, None, None]

    def advance(carry_state, inputs):
        query_block, key_block, value_block = (member.astype(jnp.float32) for member in inputs)
        local_scores = jnp.einsum('qhd,khd->hqk', query_block, key_block) * within
        intra_out = jnp.einsum('hqk,khv->hqv', rounded(local_scores), value_block)
        carried = jnp.einsum('qhd,hdv->hqv', query_block, carry_state, precision=lax.Precision.HIGHEST) * query_decay
        carry_state = carry_state * block_decay + jnp.einsum('khd,khv->hdv', key_block * key_decay, value_block, precision=lax.Precision.HIGHEST)
        normed = normalize(intra_out + carried, state_gain.reshape(HR, 1, DR))
        return (carry_state, normed.transpose(1, 0, 2).reshape(TOK_DEV, HR * DR).astype(jnp.bfloat16))
    initial = jnp.zeros((HR, DR, DR), jnp.float32)
    _, outputs = lax.scan(advance, initial, (to_blocks(ret_query), to_blocks(ret_keys), to_blocks(ret_values)))
    return outputs.reshape(length, HR * DR)

def reference(tokens, norm_gain, query_weight, key_weight, value_weight, state_query, state_key, state_value, map_lambda, diff_gain, decay_rate, state_gain, out_weight):

    def one_sequence(sequence):
        tok_float = sequence.astype(jnp.float32)
        normed = normalize(tok_float, norm_gain).astype(jnp.bfloat16)

        def project(weight):
            return jnp.dot(normed, weight, preferred_element_type=jnp.float32).astype(jnp.bfloat16)
        attended = differential(project(query_weight), project(key_weight), project(value_weight), map_lambda, diff_gain)
        retained = retention(project(state_query), project(state_key), project(state_value), decay_rate, state_gain)
        joined = jnp.concatenate([attended, retained], axis=1)
        return jnp.dot(joined, out_weight, preferred_element_type=jnp.float32).astype(jnp.bfloat16)
    return lax.map(one_sequence, tokens)
```

```python
import functools

import jax
import jax.numpy as jnp
from jax import lax
from jax.experimental import pallas as pl
from jax.experimental.pallas import tpu as pltpu
from jax.sharding import PartitionSpec as P

DK = 64
DV = 128
DR = 128


epsilon = 1e-05
branch_scale = 0.8
masked_score = -1e30


def from_behind(x, axis, by):
    size = lax.axis_size(axis)
    pairs = [(i, i + by) for i in range(size) if 0 <= i + by < size]
    return lax.ppermute(x, axis, pairs)


def entering(x, axis, join, neutral):
    place = lax.axis_index(axis)
    gathered = jax.tree.map(
        lambda a, kind: lax.all_gather(a.astype(kind), axis), x, (jnp.bfloat16, jnp.bfloat16)
    )
    state = jax.tree.map(lambda a, e: jnp.zeros_like(a) + jnp.asarray(e, a.dtype), x, neutral)

    def one(turn, state):
        return join(
            state,
            jax.tree.map(
                lambda a, own: lax.dynamic_index_in_dim(a, turn, 0, False).astype(own.dtype),
                gathered,
                x,
            ),
        )

    return lax.fori_loop(0, place, one, state)


def attend(att_query, att_keys, att_values, map_lambda, diff_gain):
    tok_rows = att_query.shape[0]
    head_count = map_lambda.shape[0]
    key_width = att_keys.shape[1]
    query_heads = att_query.reshape(tok_rows, head_count, 2, DK)
    sp_index = lax.axis_index("sp")
    query_place = sp_index * tok_rows + jnp.arange(tok_rows)
    score_scale = DK ** (-0.5)

    def absorb_block(running, inputs):
        key_block, key_place = inputs
        key_heads = key_block[:, :key_width].reshape(tok_rows, head_count, 2, DK)
        value_heads = key_block[:, key_width:].reshape(tok_rows, head_count, DV)
        scores = (
            jnp.einsum(
                "qhmd,khmd->mhqk", query_heads, key_heads, preferred_element_type=jnp.float32
            )
            * score_scale
        )
        causal = key_place[None, :] <= query_place[:, None]
        row_peak, totals, summed = running
        new_peak = jnp.maximum(row_peak, jnp.max(jnp.where(causal, scores, masked_score), axis=-1))
        weights = jnp.where(causal, jnp.exp(scores - new_peak[..., None]), 0.0)
        factor = jnp.exp(row_peak - new_peak)
        totals = totals * factor + jnp.sum(weights, axis=-1)
        summed = summed * factor[..., None] + jnp.einsum(
            "mhqk,khv->mhqv",
            weights.astype(jnp.bfloat16),
            value_heads,
            preferred_element_type=jnp.float32,
        )
        return ((new_peak, totals, summed), None)

    def absorb(running, pieces, first_row):
        piece_rows = pieces.shape[0]
        stacked = pieces.reshape(piece_rows // tok_rows, tok_rows, pieces.shape[1])
        places = (first_row + jnp.arange(piece_rows)).reshape(piece_rows // tok_rows, tok_rows)
        return lax.scan(absorb_block, running, (stacked, places))[0]

    starting = (
        jnp.full((2, head_count, tok_rows), masked_score, jnp.float32),
        jnp.zeros((2, head_count, tok_rows), jnp.float32),
        jnp.zeros((2, head_count, tok_rows, DV), jnp.float32),
    )
    joined_kv = jnp.concatenate([att_keys, att_values], axis=1)
    first_state = absorb(starting, joined_kv, sp_index * tok_rows)

    def relay_step(step_index, relay_state):
        running, moving = relay_state
        moving = from_behind(moving, "sp", 1)
        first_row = (sp_index - step_index) * tok_rows
        running = lax.cond(
            first_row >= 0,
            lambda holding: absorb(holding, moving, first_row),
            lambda holding: holding,
            running,
        )
        return (running, moving)

    running, _ = lax.fori_loop(1, lax.axis_size("sp"), relay_step, (first_state, joined_kv))
    row_peak, totals, summed = running
    averaged = summed / totals[..., None]
    differ = averaged[0] - map_lambda[:, None, None] * averaged[1]
    normed = differ * lax.rsqrt(jnp.mean(differ * differ, axis=-1, keepdims=True) + epsilon)
    normed = normed * diff_gain.reshape(head_count, 1, DV) * branch_scale
    return normed.transpose(1, 0, 2).reshape(tok_rows, head_count * DV).astype(jnp.bfloat16)


def retain(ret_query, ret_keys, ret_values, decay_rate, state_gain):
    tok_rows = ret_query.shape[0]
    head_count = decay_rate.shape[0]
    query_heads = ret_query.reshape(tok_rows, head_count, DR)
    key_heads = ret_keys.reshape(tok_rows, head_count, DR)
    value_heads = ret_values.reshape(tok_rows, head_count, DR)
    position = jnp.arange(tok_rows).astype(jnp.float32)
    distance = position[:, None] - position[None, :]
    decay_col = decay_rate[:, None, None]
    within = jnp.where(distance >= 0, jnp.exp(-decay_col * jnp.maximum(distance, 0.0)), 0.0)
    local_scores = (
        jnp.einsum("qhd,khd->hqk", query_heads, key_heads, preferred_element_type=jnp.float32)
        * within
    )
    intra_out = jnp.einsum(
        "hqk,khv->hqv",
        local_scores.astype(jnp.bfloat16),
        value_heads,
        preferred_element_type=jnp.float32,
    )
    key_decayed = key_heads.astype(jnp.float32) * jnp.exp(
        -decay_rate[None, :, None] * (tok_rows - 1.0 - position)[:, None, None]
    )
    own_state = jnp.einsum(
        "khd,khv->hdv",
        key_decayed,
        value_heads.astype(jnp.float32),
        precision=lax.Precision.HIGHEST,
    )
    block_decay = jnp.exp(-decay_rate * tok_rows)

    def link_states(earlier, later):
        return (earlier[0] * later[1][:, None, None] + later[0], earlier[1] * later[1])

    identity = (jnp.zeros_like(own_state), jnp.ones_like(block_decay))
    incoming, _ = entering((own_state, block_decay), "sp", link_states, identity)
    carried = jnp.einsum(
        "qhd,hdv->hqv", query_heads.astype(jnp.float32), incoming, precision=lax.Precision.HIGHEST
    )
    carried = carried * jnp.exp(-decay_col * (position + 1.0)[None, :, None])
    combined = intra_out + carried
    normed = combined * lax.rsqrt(jnp.mean(combined * combined, axis=-1, keepdims=True) + epsilon)
    normed = normed * state_gain.reshape(head_count, 1, DR)
    return normed.transpose(1, 0, 2).reshape(tok_rows, head_count * DR).astype(jnp.bfloat16)


def spread_body(
    tokens,
    norm_gain,
    query_weight,
    key_weight,
    value_weight,
    state_query,
    state_key,
    state_value,
    map_lambda,
    diff_gain,
    decay_rate,
    state_gain,
    out_weight,
):
    gathered = lax.all_gather(tokens[0], "tp", axis=1, tiled=True)
    tok_float = gathered.astype(jnp.float32)
    normed = tok_float * lax.rsqrt(
        jnp.mean(tok_float * tok_float, axis=-1, keepdims=True) + epsilon
    )
    normed = (normed * norm_gain).astype(jnp.bfloat16)
    pieces = (
        lax.all_gather(query_weight, "fs", axis=0, tiled=True),
        lax.all_gather(key_weight, "fs", axis=0, tiled=True),
        lax.all_gather(value_weight, "fs", axis=0, tiled=True),
        lax.all_gather(state_query, "fs", axis=0, tiled=True),
        lax.all_gather(state_key, "fs", axis=0, tiled=True),
        lax.all_gather(state_value, "fs", axis=0, tiled=True),
    )
    projected = tuple(
        (jnp.dot(normed, row_block, preferred_element_type=jnp.float32) for row_block in pieces)
    )
    att_query, att_keys, att_values, ret_query, ret_keys, ret_values = (
        member.astype(jnp.bfloat16) for member in projected
    )
    attended = attend(att_query, att_keys, att_values, map_lambda, diff_gain)
    retained = retain(ret_query, ret_keys, ret_values, decay_rate, state_gain)
    joined = jnp.concatenate([attended, retained], axis=1)
    diff_width = attended.shape[1]
    ret_width = retained.shape[1]
    tp_count = lax.axis_size("tp")
    tp_index = lax.axis_index("tp")
    own_rows = jnp.concatenate(
        [
            lax.dynamic_slice_in_dim(out_weight, tp_index * diff_width, diff_width, 0),
            lax.dynamic_slice_in_dim(
                out_weight, tp_count * diff_width + tp_index * ret_width, ret_width, 0
            ),
        ],
        axis=0,
    )
    output = lax.psum_scatter(
        jnp.dot(joined, own_rows, preferred_element_type=jnp.float32).astype(jnp.bfloat16),
        "tp",
        scatter_dimension=0,
        tiled=True,
    )
    return output[None]


def row_product(a, b):
    return lax.dot_general(a, b, (((1,), (1,)), ((), ())), preferred_element_type=jnp.float32)


def mixers_kernel(block, heads, proj, lam_ref, dgain_ref, rate_ref, sgain_ref, out):
    length = proj.shape[0]
    group = heads * DV
    f32, bf16 = jnp.float32, jnp.bfloat16
    row = lax.broadcasted_iota(jnp.int32, (block, block), 0)
    col = lax.broadcasted_iota(jnp.int32, (block, block), 1)
    causal = col <= row
    lane = lax.broadcasted_iota(jnp.int32, (block, 2 * DK), 1)
    position = lax.broadcasted_iota(jnp.int32, (block, 1), 0).astype(f32)

    def part(kind, head, first, count):
        return proj[first : first + count, kind * group + head * DV : kind * group + head * DV + DV]

    for head in range(heads):
        spot = slice(head * DV, head * DV + DV)
        lam = lam_ref[:, head : head + 1]
        rate = rate_ref[:, head : head + 1]
        gain = dgain_ref[:, spot] * branch_scale
        within = jnp.where(causal, jnp.exp(-rate * jnp.maximum(row - col, 0).astype(f32)), 0.0)
        query_decay = jnp.exp(-rate * (position + 1.0))
        key_decay = jnp.exp(-rate * (block - 1.0 - position))
        block_decay = jnp.exp(-rate * block)
        state = jnp.zeros((DR, DR), f32)
        for turn in range(length // block):
            first = turn * block
            query = part(0, head, first, block) * jnp.asarray(DK ** (-0.5), bf16)
            averaged = []
            for which in range(2):
                own = jnp.where((lane >= DK) == bool(which), query, jnp.zeros_like(query))
                near = jnp.where(causal, row_product(own, part(1, head, first, block)), masked_score)
                peak = jnp.max(near, axis=1, keepdims=True)
                if first:
                    far = row_product(own, part(1, head, 0, first))
                    peak = jnp.maximum(peak, jnp.max(far, axis=1, keepdims=True))
                near = jnp.exp(near - peak)
                total = jnp.sum(near, axis=1, keepdims=True)
                summed = jnp.dot(near.astype(bf16), part(2, head, first, block), preferred_element_type=f32)
                if first:
                    far = jnp.exp(far - peak)
                    total = total + jnp.sum(far, axis=1, keepdims=True)
                    summed = summed + jnp.dot(
                        far.astype(bf16), part(2, head, 0, first), preferred_element_type=f32
                    )
                averaged.append(summed / total)
            differ = averaged[0] - lam * averaged[1]
            scaled = differ * lax.rsqrt(jnp.mean(differ * differ, axis=1, keepdims=True) + epsilon)
            out[first : first + block, spot] = (scaled * gain).astype(bf16)
            ret_query = part(3, head, first, block)
            ret_keys = part(4, head, first, block)
            ret_values = part(5, head, first, block)
            local = (row_product(ret_query, ret_keys) * within).astype(bf16)
            mixed = jnp.dot(local, ret_values, preferred_element_type=f32)
            if first:
                mixed = mixed + query_decay * jnp.dot(
                    ret_query, state.astype(bf16), preferred_element_type=f32
                )
            if first + block < length:
                decayed = (ret_keys.astype(f32) * key_decay).astype(bf16)
                state = state * block_decay + lax.dot_general(
                    decayed, ret_values, (((0,), (0,)), ((), ())), preferred_element_type=f32
                )
            scaled = mixed * lax.rsqrt(jnp.mean(mixed * mixed, axis=1, keepdims=True) + epsilon)
            out[first : first + block, group + head * DV : group + head * DV + DV] = (
                scaled * sgain_ref[:, spot]
            ).astype(bf16)


def own_heads(x, heads):
    first = lax.axis_index("sp") * heads
    return lax.dynamic_slice_in_dim(x, first, heads, 0)[None]


def mix(proj, block, heads, map_lambda, diff_gain, decay_rate, state_gain):
    length = proj.shape[0]
    vmem = pl.BlockSpec(memory_space=pltpu.VMEM)
    return pl.pallas_call(
        functools.partial(mixers_kernel, block, heads),
        out_shape=jax.ShapeDtypeStruct((length, 2 * heads * DV), jnp.bfloat16),
        in_specs=[vmem] * 5,
        out_specs=vmem,
        compiler_params=pltpu.CompilerParams(vmem_limit_bytes=48 * 1024 * 1024),
    )(
        proj,
        own_heads(map_lambda, heads),
        own_heads(diff_gain, heads * DV),
        own_heads(decay_rate, heads),
        own_heads(state_gain, heads * DR),
    )


def body(tokens, norm_gain, *rest):
    weights, (map_lambda, diff_gain, decay_rate, state_gain, out_weight) = rest[:6], rest[6:]
    sp_count = lax.axis_size("sp")
    tp_count = lax.axis_size("tp")
    if map_lambda.shape[0] % sp_count or decay_rate.shape[0] != map_lambda.shape[0]:
        return spread_body(tokens, norm_gain, *rest)
    heads = map_lambda.shape[0] // sp_count
    block = tokens.shape[1]
    width = heads * DV
    place = lax.axis_index("sp")
    own = jnp.concatenate(
        [lax.dynamic_slice_in_dim(w, place * width, width, 1) for w in weights], axis=1
    )
    weight = lax.all_gather(own, "fs", axis=0, tiled=True)
    sequence = lax.all_gather(tokens[0], "sp", axis=0, tiled=True)
    sequence = lax.all_gather(sequence, "tp", axis=1, tiled=True)
    tok_float = sequence.astype(jnp.float32)
    normed = tok_float * lax.rsqrt(
        jnp.mean(tok_float * tok_float, axis=-1, keepdims=True) + epsilon
    )
    normed = (normed * norm_gain).astype(jnp.bfloat16)
    proj = jnp.dot(normed, weight, preferred_element_type=jnp.float32).astype(jnp.bfloat16)
    mine = mix(proj, block, heads, map_lambda, diff_gain, decay_rate, state_gain)
    count = sp_count * tp_count
    moved = lax.all_to_all(
        mine.reshape(count, mine.shape[0] // count, mine.shape[1]), ("sp", "tp"), 0, 0, tiled=True
    )
    rows = moved.shape[1]
    joined = moved.reshape(sp_count, tp_count, rows, 2, width).transpose(2, 3, 1, 0, 4)
    joined = joined.reshape(rows, out_weight.shape[0])
    return jnp.dot(joined, out_weight, preferred_element_type=jnp.float32).astype(jnp.bfloat16)[None]


def solution(mesh):
    placed = (
        P("fs", "sp", "tp"),
        P(),
        P("fs", "tp"),
        P("fs", "tp"),
        P("fs", "tp"),
        P("fs", "tp"),
        P("fs", "tp"),
        P("fs", "tp"),
        P("tp"),
        P("tp"),
        P("tp"),
        P("tp"),
        P(),
    )
    return jax.shard_map(
        body, mesh=mesh, in_specs=placed, out_specs=P("fs", ("sp", "tp"), None), check_vma=False
    )
```

```python
import functools

import jax
import jax.numpy as jnp
from jax import lax
from jax.experimental import pallas as pl
from jax.experimental.pallas import tpu as pltpu
from jax.sharding import PartitionSpec as P

DK = 64
DV = 128
DR = 128


epsilon = 1e-05
branch_scale = 0.8
masked_score = -1e30


def from_behind(x, axis, by):
    size = lax.axis_size(axis)
    pairs = [(i, i + by) for i in range(size) if 0 <= i + by < size]
    return lax.ppermute(x, axis, pairs)


def entering(x, axis, join, neutral):
    place = lax.axis_index(axis)
    gathered = jax.tree.map(
        lambda a, kind: lax.all_gather(a.astype(kind), axis), x, (jnp.bfloat16, jnp.bfloat16)
    )
    state = jax.tree.map(lambda a, e: jnp.zeros_like(a) + jnp.asarray(e, a.dtype), x, neutral)

    def one(turn, state):
        return join(
            state,
            jax.tree.map(
                lambda a, own: lax.dynamic_index_in_dim(a, turn, 0, False).astype(own.dtype),
                gathered,
                x,
            ),
        )

    return lax.fori_loop(0, place, one, state)


def attend(att_query, att_keys, att_values, map_lambda, diff_gain):
    tok_rows = att_query.shape[0]
    head_count = map_lambda.shape[0]
    key_width = att_keys.shape[1]
    query_heads = att_query.reshape(tok_rows, head_count, 2, DK)
    sp_index = lax.axis_index("sp")
    query_place = sp_index * tok_rows + jnp.arange(tok_rows)
    score_scale = DK ** (-0.5)

    def absorb_block(running, inputs):
        key_block, key_place = inputs
        key_heads = key_block[:, :key_width].reshape(tok_rows, head_count, 2, DK)
        value_heads = key_block[:, key_width:].reshape(tok_rows, head_count, DV)
        scores = (
            jnp.einsum(
                "qhmd,khmd->mhqk", query_heads, key_heads, preferred_element_type=jnp.float32
            )
            * score_scale
        )
        causal = key_place[None, :] <= query_place[:, None]
        row_peak, totals, summed = running
        new_peak = jnp.maximum(row_peak, jnp.max(jnp.where(causal, scores, masked_score), axis=-1))
        weights = jnp.where(causal, jnp.exp(scores - new_peak[..., None]), 0.0)
        factor = jnp.exp(row_peak - new_peak)
        totals = totals * factor + jnp.sum(weights, axis=-1)
        summed = summed * factor[..., None] + jnp.einsum(
            "mhqk,khv->mhqv",
            weights.astype(jnp.bfloat16),
            value_heads,
            preferred_element_type=jnp.float32,
        )
        return ((new_peak, totals, summed), None)

    def absorb(running, pieces, first_row):
        piece_rows = pieces.shape[0]
        stacked = pieces.reshape(piece_rows // tok_rows, tok_rows, pieces.shape[1])
        places = (first_row + jnp.arange(piece_rows)).reshape(piece_rows // tok_rows, tok_rows)
        return lax.scan(absorb_block, running, (stacked, places))[0]

    starting = (
        jnp.full((2, head_count, tok_rows), masked_score, jnp.float32),
        jnp.zeros((2, head_count, tok_rows), jnp.float32),
        jnp.zeros((2, head_count, tok_rows, DV), jnp.float32),
    )
    joined_kv = jnp.concatenate([att_keys, att_values], axis=1)
    first_state = absorb(starting, joined_kv, sp_index * tok_rows)

    def relay_step(step_index, relay_state):
        running, moving = relay_state
        moving = from_behind(moving, "sp", 1)
        first_row = (sp_index - step_index) * tok_rows
        running = lax.cond(
            first_row >= 0,
            lambda holding: absorb(holding, moving, first_row),
            lambda holding: holding,
            running,
        )
        return (running, moving)

    running, _ = lax.fori_loop(1, lax.axis_size("sp"), relay_step, (first_state, joined_kv))
    row_peak, totals, summed = running
    averaged = summed / totals[..., None]
    differ = averaged[0] - map_lambda[:, None, None] * averaged[1]
    normed = differ * lax.rsqrt(jnp.mean(differ * differ, axis=-1, keepdims=True) + epsilon)
    normed = normed * diff_gain.reshape(head_count, 1, DV) * branch_scale
    return normed.transpose(1, 0, 2).reshape(tok_rows, head_count * DV).astype(jnp.bfloat16)


def retain(ret_query, ret_keys, ret_values, decay_rate, state_gain):
    tok_rows = ret_query.shape[0]
    head_count = decay_rate.shape[0]
    query_heads = ret_query.reshape(tok_rows, head_count, DR)
    key_heads = ret_keys.reshape(tok_rows, head_count, DR)
    value_heads = ret_values.reshape(tok_rows, head_count, DR)
    position = jnp.arange(tok_rows).astype(jnp.float32)
    distance = position[:, None] - position[None, :]
    decay_col = decay_rate[:, None, None]
    within = jnp.where(distance >= 0, jnp.exp(-decay_col * jnp.maximum(distance, 0.0)), 0.0)
    local_scores = (
        jnp.einsum("qhd,khd->hqk", query_heads, key_heads, preferred_element_type=jnp.float32)
        * within
    )
    intra_out = jnp.einsum(
        "hqk,khv->hqv",
        local_scores.astype(jnp.bfloat16),
        value_heads,
        preferred_element_type=jnp.float32,
    )
    key_decayed = key_heads.astype(jnp.float32) * jnp.exp(
        -decay_rate[None, :, None] * (tok_rows - 1.0 - position)[:, None, None]
    )
    own_state = jnp.einsum(
        "khd,khv->hdv",
        key_decayed,
        value_heads.astype(jnp.float32),
        precision=lax.Precision.HIGHEST,
    )
    block_decay = jnp.exp(-decay_rate * tok_rows)

    def link_states(earlier, later):
        return (earlier[0] * later[1][:, None, None] + later[0], earlier[1] * later[1])

    identity = (jnp.zeros_like(own_state), jnp.ones_like(block_decay))
    incoming, _ = entering((own_state, block_decay), "sp", link_states, identity)
    carried = jnp.einsum(
        "qhd,hdv->hqv", query_heads.astype(jnp.float32), incoming, precision=lax.Precision.HIGHEST
    )
    carried = carried * jnp.exp(-decay_col * (position + 1.0)[None, :, None])
    combined = intra_out + carried
    normed = combined * lax.rsqrt(jnp.mean(combined * combined, axis=-1, keepdims=True) + epsilon)
    normed = normed * state_gain.reshape(head_count, 1, DR)
    return normed.transpose(1, 0, 2).reshape(tok_rows, head_count * DR).astype(jnp.bfloat16)


def spread_body(
    tokens,
    norm_gain,
    query_weight,
    key_weight,
    value_weight,
    state_query,
    state_key,
    state_value,
    map_lambda,
    diff_gain,
    decay_rate,
    state_gain,
    out_weight,
):
    gathered = lax.all_gather(tokens[0], "tp", axis=1, tiled=True)
    tok_float = gathered.astype(jnp.float32)
    normed = tok_float * lax.rsqrt(
        jnp.mean(tok_float * tok_float, axis=-1, keepdims=True) + epsilon
    )
    normed = (normed * norm_gain).astype(jnp.bfloat16)
    pieces = (
        lax.all_gather(query_weight, "fs", axis=0, tiled=True),
        lax.all_gather(key_weight, "fs", axis=0, tiled=True),
        lax.all_gather(value_weight, "fs", axis=0, tiled=True),
        lax.all_gather(state_query, "fs", axis=0, tiled=True),
        lax.all_gather(state_key, "fs", axis=0, tiled=True),
        lax.all_gather(state_value, "fs", axis=0, tiled=True),
    )
    projected = tuple(
        (jnp.dot(normed, row_block, preferred_element_type=jnp.float32) for row_block in pieces)
    )
    att_query, att_keys, att_values, ret_query, ret_keys, ret_values = (
        member.astype(jnp.bfloat16) for member in projected
    )
    attended = attend(att_query, att_keys, att_values, map_lambda, diff_gain)
    retained = retain(ret_query, ret_keys, ret_values, decay_rate, state_gain)
    joined = jnp.concatenate([attended, retained], axis=1)
    diff_width = attended.shape[1]
    ret_width = retained.shape[1]
    tp_count = lax.axis_size("tp")
    tp_index = lax.axis_index("tp")
    own_rows = jnp.concatenate(
        [
            lax.dynamic_slice_in_dim(out_weight, tp_index * diff_width, diff_width, 0),
            lax.dynamic_slice_in_dim(
                out_weight, tp_count * diff_width + tp_index * ret_width, ret_width, 0
            ),
        ],
        axis=0,
    )
    output = lax.psum_scatter(
        jnp.dot(joined, own_rows, preferred_element_type=jnp.float32).astype(jnp.bfloat16),
        "tp",
        scatter_dimension=0,
        tiled=True,
    )
    return output[None]


def row_product(a, b):
    return lax.dot_general(a, b, (((1,), (1,)), ((), ())), preferred_element_type=jnp.float32)


def mixers_kernel(block, heads, proj, lam_ref, dgain_ref, rate_ref, sgain_ref, out):
    length = proj.shape[0]
    group = heads * DV
    f32, bf16 = jnp.float32, jnp.bfloat16
    row = lax.broadcasted_iota(jnp.int32, (block, block), 0)
    col = lax.broadcasted_iota(jnp.int32, (block, block), 1)
    causal = col <= row
    lane = lax.broadcasted_iota(jnp.int32, (block, 2 * DK), 1)
    position = lax.broadcasted_iota(jnp.int32, (block, 1), 0).astype(f32)

    def part(kind, head, first, count):
        return proj[first : first + count, kind * group + head * DV : kind * group + head * DV + DV]

    for head in range(heads):
        spot = slice(head * DV, head * DV + DV)
        lam = lam_ref[:, head : head + 1]
        rate = rate_ref[:, head : head + 1]
        gain = dgain_ref[:, spot] * branch_scale
        within = jnp.where(causal, jnp.exp(-rate * jnp.maximum(row - col, 0).astype(f32)), 0.0)
        query_decay = jnp.exp(-rate * (position + 1.0))
        key_decay = jnp.exp(-rate * (block - 1.0 - position))
        block_decay = jnp.exp(-rate * block)
        state = jnp.zeros((DR, DR), f32)
        for turn in range(length // block):
            first = turn * block
            query = part(0, head, first, block) * jnp.asarray(DK ** (-0.5), bf16)
            averaged = []
            for which in range(2):
                own = jnp.where((lane >= DK) == bool(which), query, jnp.zeros_like(query))
                near = jnp.where(causal, row_product(own, part(1, head, first, block)), masked_score)
                peak = jnp.max(near, axis=1, keepdims=True)
                if first:
                    far = row_product(own, part(1, head, 0, first))
                    peak = jnp.maximum(peak, jnp.max(far, axis=1, keepdims=True))
                near = jnp.exp(near - peak)
                total = jnp.sum(near, axis=1, keepdims=True)
                summed = jnp.dot(near.astype(bf16), part(2, head, first, block), preferred_element_type=f32)
                if first:
                    far = jnp.exp(far - peak)
                    total = total + jnp.sum(far, axis=1, keepdims=True)
                    summed = summed + jnp.dot(
                        far.astype(bf16), part(2, head, 0, first), preferred_element_type=f32
                    )
                averaged.append(summed / total)
            differ = averaged[0] - lam * averaged[1]
            scaled = differ * lax.rsqrt(jnp.mean(differ * differ, axis=1, keepdims=True) + epsilon)
            out[first : first + block, spot] = (scaled * gain).astype(bf16)
            ret_query = part(3, head, first, block)
            ret_keys = part(4, head, first, block)
            ret_values = part(5, head, first, block)
            local = (row_product(ret_query, ret_keys) * within).astype(bf16)
            mixed = jnp.dot(local, ret_values, preferred_element_type=f32)
            if first:
                mixed = mixed + query_decay * jnp.dot(
                    ret_query, state.astype(bf16), preferred_element_type=f32
                )
            if first + block < length:
                decayed = (ret_keys.astype(f32) * key_decay).astype(bf16)
                state = state * block_decay + lax.dot_general(
                    decayed, ret_values, (((0,), (0,)), ((), ())), preferred_element_type=f32
                )
            scaled = mixed * lax.rsqrt(jnp.mean(mixed * mixed, axis=1, keepdims=True) + epsilon)
            out[first : first + block, group + head * DV : group + head * DV + DV] = (
                scaled * sgain_ref[:, spot]
            ).astype(bf16)


def own_heads(x, heads):
    first = lax.axis_index("sp") * heads
    return lax.dynamic_slice_in_dim(x, first, heads, 0)[None]


def mix(proj, block, heads, map_lambda, diff_gain, decay_rate, state_gain):
    length = proj.shape[0]
    vmem = pl.BlockSpec(memory_space=pltpu.VMEM)
    return pl.pallas_call(
        functools.partial(mixers_kernel, block, heads),
        out_shape=jax.ShapeDtypeStruct((length, 2 * heads * DV), jnp.bfloat16),
        in_specs=[vmem] * 5,
        out_specs=vmem,
        compiler_params=pltpu.CompilerParams(vmem_limit_bytes=48 * 1024 * 1024),
    )(
        proj,
        own_heads(map_lambda, heads),
        own_heads(diff_gain, heads * DV),
        own_heads(decay_rate, heads),
        own_heads(state_gain, heads * DR),
    )


MESH = pl.DeviceIdType.MESH


def greet(peers):
    barrier = pltpu.get_barrier_semaphore()
    count = 0
    for peer, present in peers:
        if present is None:
            pl.semaphore_signal(barrier, inc=1, device_id=peer, device_id_type=MESH)
            count = count + 1
        else:

            @pl.when(present)
            def _():
                pl.semaphore_signal(barrier, inc=1, device_id=peer, device_id_type=MESH)

            count = count + jnp.where(present, 1, 0)
    pl.semaphore_wait(barrier, count)


def project_kernel(
    line,
    tokens,
    gain,
    w0,
    w1,
    w2,
    w3,
    w4,
    w5,
    proj,
    seq,
    weight,
    local_sem,
    wsend,
    wrecv,
    lsend,
    lrecv,
    psend,
    precv,
):
    weights = (w0, w1, w2, w3, w4, w5)
    kinds = len(weights)
    half_kinds = kinds // 2
    z, f, c = lax.axis_index("sp"), lax.axis_index("fs"), lax.axis_index("tp")
    block, half = tokens.shape
    depth = w0.shape[0]
    width = weight.shape[1] // kinds
    near = ({"fs": f ^ 1}, {"fs": f ^ 2})
    whose = (f ^ 1, f ^ 2, f ^ 3)
    greet(
        [
            (near[0], None),
            (near[1], None),
            ({"tp": 1 - c}, None),
            ({"sp": jnp.minimum(z + 1, line - 1)}, z + 1 < line),
            ({"sp": jnp.maximum(z - 1, 0)}, z > 0),
        ]
    )

    def held(b, side):
        return seq.at[
            pl.ds(pl.multiple_of(b * block, block), block),
            pl.ds(pl.multiple_of(side * half, half), half),
        ]

    def stored(owner, kind):
        return weight.at[
            pl.ds(pl.multiple_of(owner * depth, depth), depth), kind * width : (kind + 1) * width
        ]

    def slot(e):
        if isinstance(e, int) and e == 0:
            return z
        up = (e - 1) % 2 == 0
        s = (e - 1) // 2
        return jnp.where(up, z - 1 - s, z + 1 + s)

    def along(e, b, source=None):
        up = (e - 1) % 2 == 0
        target = jnp.where(up, z + 1, z - 1)
        return pltpu.make_async_remote_copy(
            src_ref=held(b, c) if source is None else source,
            dst_ref=held(b, c),
            send_sem=lsend.at[e],
            recv_sem=lrecv.at[e],
            device_id={"sp": jnp.clip(target, 0, line - 1)},
            device_id_type=MESH,
        ), (target >= 0) & (target < line)

    def across(e, b, side, source=None):
        return pltpu.make_async_remote_copy(
            src_ref=held(b, side) if source is None else source,
            dst_ref=held(b, side),
            send_sem=psend.at[e],
            recv_sem=precv.at[e],
            device_id={"tp": 1 - c},
            device_id_type=MESH,
        )

    for e in (1, 2):
        copy, present = along(e, z, tokens)

        @pl.when(present)
        def _():
            copy.start()

    def own_columns(kind):
        return weights[kind].at[:, pl.ds(pl.multiple_of(z * width, width), width)]

    def spread(way, kind, source, owner, index):
        return pltpu.make_async_remote_copy(
            src_ref=source,
            dst_ref=stored(owner, kind),
            send_sem=wsend.at[way, index],
            recv_sem=wrecv.at[2 if index >= kinds else way, kind],
            device_id=near[way],
            device_id_type=MESH,
        )

    sends = []
    for turn in range(kinds):
        for way in range(2):
            kind = (turn + way * half_kinds) % kinds
            copy = spread(way, kind, own_columns(kind), f, kind)
            copy.start()
            sends.append(copy)
    across(0, z, c, tokens).start()
    locals_ = [pltpu.make_async_copy(tokens, held(z, c), local_sem.at[kinds])]
    for kind in range(kinds):
        locals_.append(pltpu.make_async_copy(own_columns(kind), stored(f, kind), local_sem.at[kind]))
    for copy in locals_:
        copy.start()

    def arrived(relation, kind):
        pltpu.make_async_remote_copy(
            src_ref=stored(whose[relation], kind),
            dst_ref=stored(whose[relation], kind),
            send_sem=wsend.at[0, kind],
            recv_sem=wrecv.at[relation, kind],
            device_id=near[0],
            device_id_type=MESH,
        ).wait_recv()

    for turn in range(half_kinds):
        for way in range(2):
            kind = turn + way * half_kinds
            arrived(way, kind)
            copy = spread(1 - way, kind, stored(whose[way], kind), whose[way], kinds + turn)
            copy.start()
            sends.append(copy)

    def take(s):
        for e in (1 + 2 * s, 2 + 2 * s):
            b = slot(e)

            @pl.when((b >= 0) & (b < line))
            def _():
                copy, _ = along(e, b)
                copy.wait_recv()
                if s + 1 < line - 1:
                    onward, present = along(e + 2, b)

                    @pl.when(present)
                    def _():
                        onward.start()

                across(e, b, c).start()

    def process(b):
        rows = pl.ds(pl.multiple_of(b * block, block), block)
        x = seq[rows, :].astype(jnp.float32)
        scaled = x * lax.rsqrt(jnp.mean(x * x, axis=1, keepdims=True) + epsilon)
        normed = (scaled * gain[...]).astype(jnp.bfloat16)
        proj[rows, :] = jnp.dot(normed, weight[...], preferred_element_type=jnp.float32).astype(
            jnp.bfloat16
        )

    def handle(e, carry):
        up = (e - 1) % 2 == 0
        s = (e - 1) // 2
        b = jnp.where(e == 0, z, jnp.where(up, z - 1 - s, z + 1 + s))

        @pl.when((b >= 0) & (b < line))
        def _():
            across(e, b, 1 - c).wait_recv()
            process(b)

        return carry

    for s in range(line - 2):
        take(s)
    for copy in locals_:
        copy.wait()
    for kind in range(kinds):
        for relation in range(3):
            if relation == 2 or not (relation * half_kinds <= kind < (relation + 1) * half_kinds):
                arrived(relation, kind)
    events = 2 * line - 1
    lax.fori_loop(0, events - 2, handle, 0)
    take(line - 2)
    lax.fori_loop(events - 2, events, handle, 0)

    for copy in sends:
        copy.wait_send()
    across(0, z, c, tokens).wait_send()
    for e in (1, 2):
        copy, present = along(e, z, tokens)

        @pl.when(present)
        def _():
            copy.wait_send()

    for s in range(line - 1):
        for e in (1 + 2 * s, 2 + 2 * s):
            b = slot(e)

            @pl.when((b >= 0) & (b < line))
            def _():
                across(e, b, c).wait_send()
                if s + 1 < line - 1:
                    onward, present = along(e + 2, b)

                    @pl.when(present)
                    def _():
                        onward.wait_send()


def gather_and_project(tokens, norm_gain, weights, line, width):
    block, half = tokens.shape
    kinds = len(weights)
    model = norm_gain.shape[0]
    anywhere = pl.BlockSpec(memory_space=pl.ANY)
    vmem = pl.BlockSpec(memory_space=pltpu.VMEM)
    events = 2 * line - 1
    dma = pltpu.SemaphoreType.DMA
    return pl.pallas_call(
        functools.partial(project_kernel, line),
        out_shape=jax.ShapeDtypeStruct((line * block, kinds * width), jnp.bfloat16),
        in_specs=[anywhere, vmem] + [anywhere] * kinds,
        out_specs=vmem,
        scratch_shapes=[
            pltpu.VMEM((line * block, model), jnp.bfloat16),
            pltpu.VMEM((model, kinds * width), jnp.bfloat16),
            dma((kinds + 1,)),
            dma((2, kinds + kinds // 2)),
            dma((3, kinds)),
            dma((events,)),
            dma((events,)),
            dma((events,)),
            dma((events,)),
        ],
        compiler_params=pltpu.CompilerParams(
            collective_id=0, has_side_effects=True, vmem_limit_bytes=40 * 1024 * 1024
        ),
    )(tokens, norm_gain[None], *weights)


def output_kernel(line, pair, mine, out_weight, result, joined, held, wsem, osem, send, recv):
    z, c = lax.axis_index("sp"), lax.axis_index("tp")
    count = line * pair
    me = z * pair + c
    rows = result.shape[0]
    width = mine.shape[1] // 2
    fetch = pltpu.make_async_copy(out_weight, held, wsem)
    fetch.start()
    peers = []
    for turn in range(1, count):
        other = (me + turn) % count
        peers.append((other, {"sp": other // pair, "tp": other % pair}))
    greet([(where, None) for _, where in peers])

    def place(source, which):
        first = which * (held.shape[0] // 2) + ((source % pair) * line + source // pair) * width
        return joined.at[:, pl.ds(pl.multiple_of(first, width), width)]

    def piece(target, which):
        return mine.at[
            pl.ds(pl.multiple_of(target * rows, rows), rows), which * width : (which + 1) * width
        ]

    def moved(turn, other, where, which, source):
        return pltpu.make_async_remote_copy(
            src_ref=piece(other, which),
            dst_ref=place(source, which),
            send_sem=send.at[turn, which],
            recv_sem=recv.at[turn, which],
            device_id=where,
            device_id_type=MESH,
        )

    for turn, (other, where) in enumerate(peers):
        for which in range(2):
            moved(turn, other, where, which, me).start()
    own = [pltpu.make_async_copy(piece(me, w), place(me, w), osem.at[w]) for w in range(2)]
    for copy in own:
        copy.start()
    for copy in own:
        copy.wait()
    fetch.wait()
    for turn, (other, where) in enumerate(peers):
        source = (me + count - turn - 1) % count
        for which in range(2):
            moved(turn, other, where, which, source).wait_recv()
    tile = 512

    def one(turn, carry):
        columns = pl.ds(pl.multiple_of(turn * tile, tile), tile)
        result[:, columns] = jnp.dot(
            joined[...], held[:, columns], preferred_element_type=jnp.float32
        ).astype(jnp.bfloat16)
        return carry

    lax.fori_loop(0, result.shape[1] // tile, one, 0)
    for turn, (other, where) in enumerate(peers):
        for which in range(2):
            moved(turn, other, where, which, me).wait_send()


def exchange_and_output(mine, out_weight, line, pair):
    count = line * pair
    rows = mine.shape[0] // count
    vmem = pl.BlockSpec(memory_space=pltpu.VMEM)
    dma = pltpu.SemaphoreType.DMA
    return pl.pallas_call(
        functools.partial(output_kernel, line, pair),
        out_shape=jax.ShapeDtypeStruct((rows, out_weight.shape[1]), jnp.bfloat16),
        in_specs=[vmem, pl.BlockSpec(memory_space=pl.ANY)],
        out_specs=vmem,
        scratch_shapes=[
            pltpu.VMEM((rows, out_weight.shape[0]), jnp.bfloat16),
            pltpu.VMEM(out_weight.shape, jnp.bfloat16),
            dma,
            dma((2,)),
            dma((count - 1, 2)),
            dma((count - 1, 2)),
        ],
        compiler_params=pltpu.CompilerParams(
            collective_id=1, has_side_effects=True, vmem_limit_bytes=40 * 1024 * 1024
        ),
    )(mine, out_weight)


def body(tokens, norm_gain, *rest):
    weights, (map_lambda, diff_gain, decay_rate, state_gain, out_weight) = rest[:6], rest[6:]
    line = lax.axis_size("sp")
    pair = lax.axis_size("tp")
    local = map_lambda.shape[0]
    if local % line or decay_rate.shape[0] != local or lax.axis_size("fs") != 4 or pair != 2:
        return spread_body(tokens, norm_gain, *rest)
    heads = local // line
    proj = gather_and_project(tokens[0], norm_gain, weights, line, heads * DV)
    mine = mix(proj, tokens.shape[1], heads, map_lambda, diff_gain, decay_rate, state_gain)
    return exchange_and_output(mine, out_weight, line, pair)[None]


def solution(mesh):
    placed = (
        P("fs", "sp", "tp"),
        P(),
        P("fs", "tp"),
        P("fs", "tp"),
        P("fs", "tp"),
        P("fs", "tp"),
        P("fs", "tp"),
        P("fs", "tp"),
        P("tp"),
        P("tp"),
        P("tp"),
        P("tp"),
        P(),
    )
    return jax.shard_map(
        body, mesh=mesh, in_specs=placed, out_specs=P("fs", ("sp", "tp"), None), check_vma=False
    )
```

```python
import functools

import jax
import jax.numpy as jnp
from jax import lax
from jax.experimental import pallas as pl
from jax.experimental.pallas import tpu as pltpu
from jax.sharding import PartitionSpec as P

DK = 64
DV = 128
DR = 128


epsilon = 1e-05
branch_scale = 0.8
masked_score = -1e30


def from_behind(x, axis, by):
    size = lax.axis_size(axis)
    pairs = [(i, i + by) for i in range(size) if 0 <= i + by < size]
    return lax.ppermute(x, axis, pairs)


def entering(x, axis, join, neutral):
    place = lax.axis_index(axis)
    gathered = jax.tree.map(
        lambda a, kind: lax.all_gather(a.astype(kind), axis), x, (jnp.bfloat16, jnp.bfloat16)
    )
    state = jax.tree.map(lambda a, e: jnp.zeros_like(a) + jnp.asarray(e, a.dtype), x, neutral)

    def one(turn, state):
        return join(
            state,
            jax.tree.map(
                lambda a, own: lax.dynamic_index_in_dim(a, turn, 0, False).astype(own.dtype),
                gathered,
                x,
            ),
        )

    return lax.fori_loop(0, place, one, state)


def attend(att_query, att_keys, att_values, map_lambda, diff_gain):
    tok_rows = att_query.shape[0]
    head_count = map_lambda.shape[0]
    key_width = att_keys.shape[1]
    query_heads = att_query.reshape(tok_rows, head_count, 2, DK)
    sp_index = lax.axis_index("sp")
    query_place = sp_index * tok_rows + jnp.arange(tok_rows)
    score_scale = DK ** (-0.5)

    def absorb_block(running, inputs):
        key_block, key_place = inputs
        key_heads = key_block[:, :key_width].reshape(tok_rows, head_count, 2, DK)
        value_heads = key_block[:, key_width:].reshape(tok_rows, head_count, DV)
        scores = (
            jnp.einsum(
                "qhmd,khmd->mhqk", query_heads, key_heads, preferred_element_type=jnp.float32
            )
            * score_scale
        )
        causal = key_place[None, :] <= query_place[:, None]
        row_peak, totals, summed = running
        new_peak = jnp.maximum(row_peak, jnp.max(jnp.where(causal, scores, masked_score), axis=-1))
        weights = jnp.where(causal, jnp.exp(scores - new_peak[..., None]), 0.0)
        factor = jnp.exp(row_peak - new_peak)
        totals = totals * factor + jnp.sum(weights, axis=-1)
        summed = summed * factor[..., None] + jnp.einsum(
            "mhqk,khv->mhqv",
            weights.astype(jnp.bfloat16),
            value_heads,
            preferred_element_type=jnp.float32,
        )
        return ((new_peak, totals, summed), None)

    def absorb(running, pieces, first_row):
        piece_rows = pieces.shape[0]
        stacked = pieces.reshape(piece_rows // tok_rows, tok_rows, pieces.shape[1])
        places = (first_row + jnp.arange(piece_rows)).reshape(piece_rows // tok_rows, tok_rows)
        return lax.scan(absorb_block, running, (stacked, places))[0]

    starting = (
        jnp.full((2, head_count, tok_rows), masked_score, jnp.float32),
        jnp.zeros((2, head_count, tok_rows), jnp.float32),
        jnp.zeros((2, head_count, tok_rows, DV), jnp.float32),
    )
    joined_kv = jnp.concatenate([att_keys, att_values], axis=1)
    first_state = absorb(starting, joined_kv, sp_index * tok_rows)

    def relay_step(step_index, relay_state):
        running, moving = relay_state
        moving = from_behind(moving, "sp", 1)
        first_row = (sp_index - step_index) * tok_rows
        running = lax.cond(
            first_row >= 0,
            lambda holding: absorb(holding, moving, first_row),
            lambda holding: holding,
            running,
        )
        return (running, moving)

    running, _ = lax.fori_loop(1, lax.axis_size("sp"), relay_step, (first_state, joined_kv))
    row_peak, totals, summed = running
    averaged = summed / totals[..., None]
    differ = averaged[0] - map_lambda[:, None, None] * averaged[1]
    normed = differ * lax.rsqrt(jnp.mean(differ * differ, axis=-1, keepdims=True) + epsilon)
    normed = normed * diff_gain.reshape(head_count, 1, DV) * branch_scale
    return normed.transpose(1, 0, 2).reshape(tok_rows, head_count * DV).astype(jnp.bfloat16)


def retain(ret_query, ret_keys, ret_values, decay_rate, state_gain):
    tok_rows = ret_query.shape[0]
    head_count = decay_rate.shape[0]
    query_heads = ret_query.reshape(tok_rows, head_count, DR)
    key_heads = ret_keys.reshape(tok_rows, head_count, DR)
    value_heads = ret_values.reshape(tok_rows, head_count, DR)
    position = jnp.arange(tok_rows).astype(jnp.float32)
    distance = position[:, None] - position[None, :]
    decay_col = decay_rate[:, None, None]
    within = jnp.where(distance >= 0, jnp.exp(-decay_col * jnp.maximum(distance, 0.0)), 0.0)
    local_scores = (
        jnp.einsum("qhd,khd->hqk", query_heads, key_heads, preferred_element_type=jnp.float32)
        * within
    )
    intra_out = jnp.einsum(
        "hqk,khv->hqv",
        local_scores.astype(jnp.bfloat16),
        value_heads,
        preferred_element_type=jnp.float32,
    )
    key_decayed = key_heads.astype(jnp.float32) * jnp.exp(
        -decay_rate[None, :, None] * (tok_rows - 1.0 - position)[:, None, None]
    )
    own_state = jnp.einsum(
        "khd,khv->hdv",
        key_decayed,
        value_heads.astype(jnp.float32),
        precision=lax.Precision.HIGHEST,
    )
    block_decay = jnp.exp(-decay_rate * tok_rows)

    def link_states(earlier, later):
        return (earlier[0] * later[1][:, None, None] + later[0], earlier[1] * later[1])

    identity = (jnp.zeros_like(own_state), jnp.ones_like(block_decay))
    incoming, _ = entering((own_state, block_decay), "sp", link_states, identity)
    carried = jnp.einsum(
        "qhd,hdv->hqv", query_heads.astype(jnp.float32), incoming, precision=lax.Precision.HIGHEST
    )
    carried = carried * jnp.exp(-decay_col * (position + 1.0)[None, :, None])
    combined = intra_out + carried
    normed = combined * lax.rsqrt(jnp.mean(combined * combined, axis=-1, keepdims=True) + epsilon)
    normed = normed * state_gain.reshape(head_count, 1, DR)
    return normed.transpose(1, 0, 2).reshape(tok_rows, head_count * DR).astype(jnp.bfloat16)


def spread_body(
    tokens,
    norm_gain,
    query_weight,
    key_weight,
    value_weight,
    state_query,
    state_key,
    state_value,
    map_lambda,
    diff_gain,
    decay_rate,
    state_gain,
    out_weight,
):
    gathered = lax.all_gather(tokens[0], "tp", axis=1, tiled=True)
    tok_float = gathered.astype(jnp.float32)
    normed = tok_float * lax.rsqrt(
        jnp.mean(tok_float * tok_float, axis=-1, keepdims=True) + epsilon
    )
    normed = (normed * norm_gain).astype(jnp.bfloat16)
    pieces = (
        lax.all_gather(query_weight, "fs", axis=0, tiled=True),
        lax.all_gather(key_weight, "fs", axis=0, tiled=True),
        lax.all_gather(value_weight, "fs", axis=0, tiled=True),
        lax.all_gather(state_query, "fs", axis=0, tiled=True),
        lax.all_gather(state_key, "fs", axis=0, tiled=True),
        lax.all_gather(state_value, "fs", axis=0, tiled=True),
    )
    projected = tuple(
        (jnp.dot(normed, row_block, preferred_element_type=jnp.float32) for row_block in pieces)
    )
    att_query, att_keys, att_values, ret_query, ret_keys, ret_values = (
        member.astype(jnp.bfloat16) for member in projected
    )
    attended = attend(att_query, att_keys, att_values, map_lambda, diff_gain)
    retained = retain(ret_query, ret_keys, ret_values, decay_rate, state_gain)
    joined = jnp.concatenate([attended, retained], axis=1)
    diff_width = attended.shape[1]
    ret_width = retained.shape[1]
    tp_count = lax.axis_size("tp")
    tp_index = lax.axis_index("tp")
    own_rows = jnp.concatenate(
        [
            lax.dynamic_slice_in_dim(out_weight, tp_index * diff_width, diff_width, 0),
            lax.dynamic_slice_in_dim(
                out_weight, tp_count * diff_width + tp_index * ret_width, ret_width, 0
            ),
        ],
        axis=0,
    )
    output = lax.psum_scatter(
        jnp.dot(joined, own_rows, preferred_element_type=jnp.float32).astype(jnp.bfloat16),
        "tp",
        scatter_dimension=0,
        tiled=True,
    )
    return output[None]


def row_product(a, b):
    return lax.dot_general(a, b, (((1,), (1,)), ((), ())), preferred_element_type=jnp.float32)


def mixers_kernel(block, heads, proj, lam_ref, dgain_ref, rate_ref, sgain_ref, out):
    length = proj.shape[0]
    group = heads * DV
    place = lax.axis_index("sp")
    f32, bf16 = jnp.float32, jnp.bfloat16
    row = lax.broadcasted_iota(jnp.int32, (block, block), 0)
    col = lax.broadcasted_iota(jnp.int32, (block, block), 1)
    causal = col <= row
    lane = lax.broadcasted_iota(jnp.int32, (block, 2 * DK), 1)
    position = lax.broadcasted_iota(jnp.int32, (block, 1), 0).astype(f32)

    def part(kind, head, first, count):
        return proj[first : first + count, kind * group + head * DV : kind * group + head * DV + DV]

    for head in range(heads):
        spot = slice(head * DV, head * DV + DV)
        lam = lam_ref[place * heads + head]
        rate = rate_ref[place * heads + head]
        mine = pl.ds(pl.multiple_of((place * heads + head) * DV, DV), DV)
        gain = dgain_ref[:, mine] * branch_scale
        within = jnp.where(causal, jnp.exp(-rate * jnp.maximum(row - col, 0).astype(f32)), 0.0)
        query_decay = jnp.exp(-rate * (position + 1.0))
        key_decay = jnp.exp(-rate * (block - 1.0 - position))
        block_decay = jnp.exp(jnp.full((1, DR), -block, f32) * rate)
        state = jnp.zeros((DR, DR), f32)
        for turn in range(length // block):
            first = turn * block
            query = part(0, head, first, block) * jnp.asarray(DK ** (-0.5), bf16)
            averaged = []
            for which in range(2):
                own = jnp.where((lane >= DK) == bool(which), query, jnp.zeros_like(query))
                near = jnp.where(causal, row_product(own, part(1, head, first, block)), masked_score)
                peak = jnp.max(near, axis=1, keepdims=True)
                if first:
                    far = row_product(own, part(1, head, 0, first))
                    peak = jnp.maximum(peak, jnp.max(far, axis=1, keepdims=True))
                near = jnp.exp(near - peak)
                total = jnp.sum(near, axis=1, keepdims=True)
                summed = jnp.dot(near.astype(bf16), part(2, head, first, block), preferred_element_type=f32)
                if first:
                    far = jnp.exp(far - peak)
                    total = total + jnp.sum(far, axis=1, keepdims=True)
                    summed = summed + jnp.dot(
                        far.astype(bf16), part(2, head, 0, first), preferred_element_type=f32
                    )
                averaged.append(summed / total)
            differ = averaged[0] - lam * averaged[1]
            scaled = differ * lax.rsqrt(jnp.mean(differ * differ, axis=1, keepdims=True) + epsilon)
            out[first : first + block, spot] = (scaled * gain).astype(bf16)
            ret_query = part(3, head, first, block)
            ret_keys = part(4, head, first, block)
            ret_values = part(5, head, first, block)
            local = (row_product(ret_query, ret_keys) * within).astype(bf16)
            mixed = jnp.dot(local, ret_values, preferred_element_type=f32)
            if first:
                mixed = mixed + query_decay * jnp.dot(
                    ret_query, state.astype(bf16), preferred_element_type=f32
                )
            if first + block < length:
                decayed = (ret_keys.astype(f32) * key_decay).astype(bf16)
                state = state * block_decay + lax.dot_general(
                    decayed, ret_values, (((0,), (0,)), ((), ())), preferred_element_type=f32
                )
            scaled = mixed * lax.rsqrt(jnp.mean(mixed * mixed, axis=1, keepdims=True) + epsilon)
            out[first : first + block, group + head * DV : group + head * DV + DV] = (
                scaled * sgain_ref[:, mine]
            ).astype(bf16)


def mix(proj, block, heads, map_lambda, diff_gain, decay_rate, state_gain):
    length = proj.shape[0]
    vmem = pl.BlockSpec(memory_space=pltpu.VMEM)
    smem = pl.BlockSpec(memory_space=pltpu.SMEM)
    return pl.pallas_call(
        functools.partial(mixers_kernel, block, heads),
        out_shape=jax.ShapeDtypeStruct((length, 2 * heads * DV), jnp.bfloat16),
        in_specs=[vmem, smem, vmem, smem, vmem],
        out_specs=vmem,
        compiler_params=pltpu.CompilerParams(vmem_limit_bytes=65000 * 1024),
    )(
        proj,
        map_lambda,
        diff_gain[None],
        decay_rate,
        state_gain[None],
    )


MESH = pl.DeviceIdType.MESH


def greet(peers):
    barrier = pltpu.get_barrier_semaphore()
    count = 0
    for peer, present in peers:
        if present is None:
            pl.semaphore_signal(barrier, inc=1, device_id=peer, device_id_type=MESH)
            count = count + 1
        else:

            @pl.when(present)
            def _():
                pl.semaphore_signal(barrier, inc=1, device_id=peer, device_id_type=MESH)

            count = count + jnp.where(present, 1, 0)
    pl.semaphore_wait(barrier, count)


def project_kernel(
    line,
    tokens,
    gain,
    w0,
    w1,
    w2,
    w3,
    w4,
    w5,
    proj,
    seq,
    weight,
    local_sem,
    wsend,
    wrecv,
    lsend,
    lrecv,
    psend,
    precv,
):
    weights = (w0, w1, w2, w3, w4, w5)
    kinds = len(weights)
    half_kinds = kinds // 2
    z, f, c = lax.axis_index("sp"), lax.axis_index("fs"), lax.axis_index("tp")
    block, half = tokens.shape
    depth = w0.shape[0]
    width = weight.shape[1] // kinds
    near = ({"fs": f ^ 1}, {"fs": f ^ 2})
    whose = (f ^ 1, f ^ 2, f ^ 3)
    greet(
        [
            (near[0], None),
            (near[1], None),
            ({"tp": 1 - c}, None),
            ({"sp": jnp.minimum(z + 1, line - 1)}, z + 1 < line),
            ({"sp": jnp.maximum(z - 1, 0)}, z > 0),
        ]
    )

    def held(b, side):
        return seq.at[
            pl.ds(pl.multiple_of(b * block, block), block),
            pl.ds(pl.multiple_of(side * half, half), half),
        ]

    def stored(owner, kind):
        return weight.at[
            pl.ds(pl.multiple_of(owner * depth, depth), depth), kind * width : (kind + 1) * width
        ]

    def slot(e):
        if isinstance(e, int) and e == 0:
            return z
        up = (e - 1) % 2 == 0
        s = (e - 1) // 2
        return jnp.where(up, z - 1 - s, z + 1 + s)

    def along(e, b, source=None):
        up = (e - 1) % 2 == 0
        target = jnp.where(up, z + 1, z - 1)
        return pltpu.make_async_remote_copy(
            src_ref=held(b, c) if source is None else source,
            dst_ref=held(b, c),
            send_sem=lsend.at[e],
            recv_sem=lrecv.at[e],
            device_id={"sp": jnp.clip(target, 0, line - 1)},
            device_id_type=MESH,
        ), (target >= 0) & (target < line)

    def across(e, b, side, source=None):
        return pltpu.make_async_remote_copy(
            src_ref=held(b, side) if source is None else source,
            dst_ref=held(b, side),
            send_sem=psend.at[e],
            recv_sem=precv.at[e],
            device_id={"tp": 1 - c},
            device_id_type=MESH,
        )

    for e in (1, 2):
        copy, present = along(e, z, tokens)

        @pl.when(present)
        def _():
            copy.start()

    def own_columns(kind):
        return weights[kind].at[:, pl.ds(pl.multiple_of(z * width, width), width)]

    def spread(way, kind, source, owner, index):
        return pltpu.make_async_remote_copy(
            src_ref=source,
            dst_ref=stored(owner, kind),
            send_sem=wsend.at[way, index],
            recv_sem=wrecv.at[2 if index >= kinds else way, kind],
            device_id=near[way],
            device_id_type=MESH,
        )

    sends = []
    for turn in range(kinds):
        for way in range(2):
            kind = (turn + way * half_kinds) % kinds
            copy = spread(way, kind, own_columns(kind), f, kind)
            copy.start()
            sends.append(copy)
    across(0, z, c, tokens).start()
    locals_ = [pltpu.make_async_copy(tokens, held(z, c), local_sem.at[kinds])]
    for kind in range(kinds):
        locals_.append(pltpu.make_async_copy(own_columns(kind), stored(f, kind), local_sem.at[kind]))
    for copy in locals_:
        copy.start()

    def arrived(relation, kind):
        pltpu.make_async_remote_copy(
            src_ref=stored(whose[relation], kind),
            dst_ref=stored(whose[relation], kind),
            send_sem=wsend.at[0, kind],
            recv_sem=wrecv.at[relation, kind],
            device_id=near[0],
            device_id_type=MESH,
        ).wait_recv()

    for turn in range(half_kinds):
        for way in range(2):
            kind = turn + way * half_kinds
            arrived(way, kind)
            copy = spread(1 - way, kind, stored(whose[way], kind), whose[way], kinds + turn)
            copy.start()
            sends.append(copy)

    def take(s):
        for e in (1 + 2 * s, 2 + 2 * s):
            b = slot(e)

            @pl.when((b >= 0) & (b < line))
            def _():
                copy, _ = along(e, b)
                copy.wait_recv()
                if s + 1 < line - 1:
                    onward, present = along(e + 2, b)

                    @pl.when(present)
                    def _():
                        onward.start()

                across(e, b, c).start()

    def process(b):
        rows = pl.ds(pl.multiple_of(b * block, block), block)
        x = seq[rows, :].astype(jnp.float32)
        scaled = x * lax.rsqrt(jnp.mean(x * x, axis=1, keepdims=True) + epsilon)
        normed = (scaled * gain[...]).astype(jnp.bfloat16)
        proj[rows, :] = jnp.dot(normed, weight[...], preferred_element_type=jnp.float32).astype(
            jnp.bfloat16
        )

    def handle(e, carry):
        up = (e - 1) % 2 == 0
        s = (e - 1) // 2
        b = jnp.where(e == 0, z, jnp.where(up, z - 1 - s, z + 1 + s))

        @pl.when((b >= 0) & (b < line))
        def _():
            across(e, b, 1 - c).wait_recv()
            process(b)

        return carry

    for s in range(line - 2):
        take(s)
    for copy in locals_:
        copy.wait()
    for kind in range(kinds):
        for relation in range(3):
            if relation == 2 or not (relation * half_kinds <= kind < (relation + 1) * half_kinds):
                arrived(relation, kind)
    events = 2 * line - 1
    lax.fori_loop(0, events - 2, handle, 0)
    take(line - 2)
    lax.fori_loop(events - 2, events, handle, 0)

    for copy in sends:
        copy.wait_send()
    across(0, z, c, tokens).wait_send()
    for e in (1, 2):
        copy, present = along(e, z, tokens)

        @pl.when(present)
        def _():
            copy.wait_send()

    for s in range(line - 1):
        for e in (1 + 2 * s, 2 + 2 * s):
            b = slot(e)

            @pl.when((b >= 0) & (b < line))
            def _():
                across(e, b, c).wait_send()
                if s + 1 < line - 1:
                    onward, present = along(e + 2, b)

                    @pl.when(present)
                    def _():
                        onward.wait_send()


def gather_and_project(tokens, norm_gain, weights, line, width):
    block, half = tokens.shape
    kinds = len(weights)
    model = norm_gain.shape[0]
    anywhere = pl.BlockSpec(memory_space=pl.ANY)
    vmem = pl.BlockSpec(memory_space=pltpu.VMEM)
    events = 2 * line - 1
    dma = pltpu.SemaphoreType.DMA
    return pl.pallas_call(
        functools.partial(project_kernel, line),
        out_shape=jax.ShapeDtypeStruct((line * block, kinds * width), jnp.bfloat16),
        in_specs=[anywhere, vmem] + [anywhere] * kinds,
        out_specs=vmem,
        scratch_shapes=[
            pltpu.VMEM((line * block, model), jnp.bfloat16),
            pltpu.VMEM((model, kinds * width), jnp.bfloat16),
            dma((kinds + 1,)),
            dma((2, kinds + kinds // 2)),
            dma((3, kinds)),
            dma((events,)),
            dma((events,)),
            dma((events,)),
            dma((events,)),
        ],
        compiler_params=pltpu.CompilerParams(
            collective_id=0, has_side_effects=True, vmem_limit_bytes=65000 * 1024
        ),
    )(tokens, norm_gain[None], *weights)


def output_kernel(line, pair, mine, out_weight, result, joined, held, wsem, osem, send, recv):
    z, c = lax.axis_index("sp"), lax.axis_index("tp")
    count = line * pair
    me = z * pair + c
    rows = result.shape[0]
    width = mine.shape[1] // 2
    fetch = pltpu.make_async_copy(out_weight, held, wsem)
    fetch.start()
    peers = []
    for turn in range(1, count):
        other = (me + turn) % count
        peers.append((other, {"sp": other // pair, "tp": other % pair}))
    greet([(where, None) for _, where in peers])

    def place(source, which):
        first = which * (held.shape[0] // 2) + ((source % pair) * line + source // pair) * width
        return joined.at[:, pl.ds(pl.multiple_of(first, width), width)]

    def piece(target, which):
        return mine.at[
            pl.ds(pl.multiple_of(target * rows, rows), rows), which * width : (which + 1) * width
        ]

    def moved(turn, other, where, which, source):
        return pltpu.make_async_remote_copy(
            src_ref=piece(other, which),
            dst_ref=place(source, which),
            send_sem=send.at[turn, which],
            recv_sem=recv.at[turn, which],
            device_id=where,
            device_id_type=MESH,
        )

    for turn, (other, where) in enumerate(peers):
        for which in range(2):
            moved(turn, other, where, which, me).start()
    own = [pltpu.make_async_copy(piece(me, w), place(me, w), osem.at[w]) for w in range(2)]
    for copy in own:
        copy.start()
    for copy in own:
        copy.wait()
    fetch.wait()
    for turn, (other, where) in enumerate(peers):
        source = (me + count - turn - 1) % count
        for which in range(2):
            moved(turn, other, where, which, source).wait_recv()
    tile = 512

    def one(turn, carry):
        columns = pl.ds(pl.multiple_of(turn * tile, tile), tile)
        result[:, columns] = jnp.dot(
            joined[...], held[:, columns], preferred_element_type=jnp.float32
        ).astype(jnp.bfloat16)
        return carry

    lax.fori_loop(0, result.shape[1] // tile, one, 0)
    for turn, (other, where) in enumerate(peers):
        for which in range(2):
            moved(turn, other, where, which, me).wait_send()


def exchange_and_output(mine, out_weight, line, pair):
    count = line * pair
    rows = mine.shape[0] // count
    vmem = pl.BlockSpec(memory_space=pltpu.VMEM)
    dma = pltpu.SemaphoreType.DMA
    return pl.pallas_call(
        functools.partial(output_kernel, line, pair),
        out_shape=jax.ShapeDtypeStruct((rows, out_weight.shape[1]), jnp.bfloat16),
        in_specs=[vmem, pl.BlockSpec(memory_space=pl.ANY)],
        out_specs=vmem,
        scratch_shapes=[
            pltpu.VMEM((rows, out_weight.shape[0]), jnp.bfloat16),
            pltpu.VMEM(out_weight.shape, jnp.bfloat16),
            dma,
            dma((2,)),
            dma((count - 1, 2)),
            dma((count - 1, 2)),
        ],
        compiler_params=pltpu.CompilerParams(
            collective_id=1, has_side_effects=True, vmem_limit_bytes=65000 * 1024
        ),
    )(mine, out_weight)


def body(tokens, norm_gain, *rest):
    weights, (map_lambda, diff_gain, decay_rate, state_gain, out_weight) = rest[:6], rest[6:]
    line = lax.axis_size("sp")
    pair = lax.axis_size("tp")
    local = map_lambda.shape[0]
    if local % line or decay_rate.shape[0] != local or lax.axis_size("fs") != 4 or pair != 2:
        return spread_body(tokens, norm_gain, *rest)
    heads = local // line
    proj = gather_and_project(tokens[0], norm_gain, weights, line, heads * DV)
    mine = mix(proj, tokens.shape[1], heads, map_lambda, diff_gain, decay_rate, state_gain)
    return exchange_and_output(mine, out_weight, line, pair)[None]


def solution(mesh):
    placed = (
        P("fs", "sp", "tp"),
        P(),
        P("fs", "tp"),
        P("fs", "tp"),
        P("fs", "tp"),
        P("fs", "tp"),
        P("fs", "tp"),
        P("fs", "tp"),
        P("tp"),
        P("tp"),
        P("tp"),
        P("tp"),
        P(),
    )
    return jax.shard_map(
        body, mesh=mesh, in_specs=placed, out_specs=P("fs", ("sp", "tp"), None), check_vma=False
    )
```
